256 devices in a mesh: gr: 2 (over z_hi), fs: 16 (over z_lo, y), tp: 8 (over x, core).
Axes of the slice: x: 4, y: 4, z: 8 (z_hi: 2, z_lo: 4; z = z_hi * 4 + z_lo), core: 2. Of those that a mesh axis runs over, the one named last changes fastest.
Arguments:
- prompt: bfloat16 [24576, 2048], P(('gr', 'fs', 'tp')), may hold values from -6 to 6
- norm_first: float32 [2048], P(('gr', 'fs')), may hold values from 0.1 to 1.9
- gate_first: float32 [2048, 5632], P(('gr', 'fs'), 'tp'), may hold values from -6 to 6
- up_first: float32 [2048, 5632], P(('gr', 'fs'), 'tp'), may hold values from -6 to 6
- down_first: float32 [2048, 5632], P(('gr', 'fs'), 'tp'), may hold values from -6 to 6
- norm_second: float32 [2048], P(('gr', 'fs')), may hold values from 0.1 to 1.9
- gate_second: float32 [2048, 5632], P(('gr', 'fs'), 'tp'), may hold values from -6 to 6
- up_second: float32 [2048, 5632], P(('gr', 'fs'), 'tp'), may hold values from -6 to 6
- down_second: float32 [2048, 5632], P(('gr', 'fs'), 'tp'), may hold values from -6 to 6
Outputs:
- served_gate_first: bfloat16 [2048, 5632], P(None, 'fs')
- served_up_first: bfloat16 [2048, 5632], P(None, 'fs')
- served_down_first: bfloat16 [2048, 5632], P(None, 'fs')
- served_gate_second: bfloat16 [2048, 5632], P(None, 'fs')
- served_up_second: bfloat16 [2048, 5632], P(None, 'fs')
- served_down_second: bfloat16 [2048, 5632], P(None, 'fs')
- result: bfloat16 [24576, 2048], P(('gr', 'fs', 'tp'))
The draws below stay inside these ranges and needn't reach their ends.
All inputs are finite; a program needn't handle non-finite values.
Results may differ from the reference program's by a relative error of at most 0.015.
Values may be sent and summed in bfloat16 or wider, within the bound.
A program may use at most 128 MiB of HBM per device.

```python
import jax
import jax.numpy as jnp
from jax import lax

D = 2048
FF = 5632
FF_BLK = 352
TOKENS = 24576


def block_scale(key, shape, cuts, least, high):
    factor_of = 1.0
    for axis_at, parts in cuts:
        heights = jax.random.uniform(jax.random.fold_in(jax.random.fold_in(key, 6), axis_at), (parts,), jnp.float32, least / len(cuts), high / len(cuts))
        factor_of = factor_of * jnp.repeat(jnp.exp(heights), shape[axis_at] // parts).reshape((-1,) + (1,) * (len(shape) - 1 - axis_at))
    return factor_of


def scatter_about(stream_key, extent, spread, most, pieces=(), kind=jnp.bfloat16):
    level = block_scale(stream_key, extent, pieces, -0.22, 0.18) if pieces else 1.0
    drawn = jax.random.normal(stream_key, extent, jnp.float32) * spread * level
    return jnp.minimum(jnp.maximum(drawn, -most), most).astype(kind)


def setup_inputs(seed: int = 0) -> dict:
    seeds = jax.random.split(jax.random.key(seed), 10)
    prompt = scatter_about(seeds[0], (TOKENS, D), 1.0, 6.0, ((0, 256),))
    norm_first = jnp.clip(1.0 + 0.18 * jax.random.normal(seeds[1], (D,), jnp.float32), 0.1, 1.9)
    gate_first = scatter_about(seeds[2], (D, FF), 1.0, 6.0, ((0, 32), (1, 8)), jnp.float32)
    up_first = scatter_about(seeds[3], (D, FF), 1.0, 6.0, ((0, 32), (1, 8)), jnp.float32)
    down_first = scatter_about(seeds[4], (D, FF), 1.0, 6.0, ((0, 32), (1, 8)), jnp.float32)
    norm_second = jnp.clip(1.0 + 0.18 * jax.random.normal(seeds[5], (D,), jnp.float32), 0.1, 1.9)
    gate_second = scatter_about(seeds[6], (D, FF), 1.0, 6.0, ((0, 32), (1, 8)), jnp.float32)
    up_second = scatter_about(seeds[7], (D, FF), 1.0, 6.0, ((0, 32), (1, 8)), jnp.float32)
    down_second = scatter_about(seeds[8], (D, FF), 1.0, 6.0, ((0, 32), (1, 8)), jnp.float32)
    return dict(prompt=prompt, norm_first=norm_first, gate_first=gate_first, up_first=up_first, down_first=down_first, norm_second=norm_second, gate_second=gate_second, up_second=up_second, down_second=down_second)


EPS = 1e-06

def fold_rows(gain, weight):
    return (gain[:, None] * weight).astype(jnp.bfloat16)

def half_step(residual, gate_weight, up_weight, down_weight):
    resid_f = residual.astype(jnp.float32)
    normed = (resid_f * lax.rsqrt(lax.optimization_barrier(jnp.mean(resid_f * resid_f, axis=-1, keepdims=True)) + EPS)).astype(jnp.bfloat16)
    gate_pre = jnp.dot(normed, gate_weight, preferred_element_type=jnp.float32) * D ** (-0.5)
    up_pre = jnp.dot(normed, up_weight, preferred_element_type=jnp.float32) * D ** (-0.5)
    hidden = (jax.nn.silu(gate_pre) * up_pre).astype(jnp.bfloat16)

    def add_block(running, block_index):
        offset = block_index * FF_BLK
        hid_block = lax.dynamic_slice_in_dim(hidden, offset, FF_BLK, 1)
        down_block = lax.dynamic_slice_in_dim(down_weight, offset, FF_BLK, 1)
        partial_sum = lax.dot_general(hid_block, down_block, (((1,), (1,)), ((), ())), preferred_element_type=jnp.float32) * FF ** (-0.5)
        partial_sum = lax.optimization_barrier(partial_sum.astype(jnp.bfloat16)).astype(jnp.float32)
        return (running + partial_sum, None)
    start_sum = jnp.zeros((residual.shape[0], D), jnp.float32)
    branch, _ = lax.scan(add_block, start_sum, jnp.arange(FF // FF_BLK, dtype=jnp.int32))
    return (resid_f + 0.5 * branch).astype(jnp.bfloat16)

def reference(prompt, norm_first, gate_first, up_first, down_first, norm_second, gate_second, up_second, down_second):
    served_gate_first = fold_rows(norm_first, gate_first)
    served_up_first = fold_rows(norm_first, up_first)
    served_down_first = down_first.astype(jnp.bfloat16)
    served_gate_second = fold_rows(norm_second, gate_second)
    served_up_second = fold_rows(norm_second, up_second)
    served_down_second = down_second.astype(jnp.bfloat16)
    middle = half_step(prompt, served_gate_first, served_up_first, served_down_first)
    result = half_step(middle, served_gate_second, served_up_second, served_down_second)
    return (served_gate_first, served_up_first, served_down_first, served_gate_second, served_up_second, served_down_second, result)
```

```python
import jax
import jax.numpy as jnp
from jax import lax
from jax.experimental import pallas as pl
from jax.experimental.pallas import tpu as pltpu
from jax.sharding import PartitionSpec as P

D = 2048
FF = 5632
EPS = 1e-06
NY, NZ, NX = 4, 8, 4
TOK = 96
HALF = 48
ROWS = 64
PIECE = 32
COLS = 704
BLK = 352
PAD = 384
PACK = 2176
GU = 1408
DN = 768
SERVED = 3 * PAD
NR = 17
LANES = ((0, 768), (768, 640), (1408, 768))
CH = 512
NCH = D // CH
IN_SCALE = D ** (-0.5)
OUT_SCALE = FF ** (-0.5)
ROUNDS = 2 * NR + 10


def kernel(
    packed,
    prompt,
    served,
    result,
    wall,
    xa,
    pre,
    hid,
    accs,
    own,
    part,
    st2,
    comb,
    cbuf,
    rbuf,
    resid,
    stage,
    load_sem,
    ring_recv,
    ring_send,
    d2d_recv,
    d2d_send,
    srecv,
    s_fwd_send,
    s_d2d_send,
    s_d2d_recv,
    ag_recv,
    ag_send,
    c_recv,
    c_send,
    r_recv,
    r_send,
):
    gr = lax.axis_index("gr")
    fs = lax.axis_index("fs")
    tp = lax.axis_index("tp")
    z_lo, y = fs // NY, fs % NY
    z = gr * 4 + z_lo
    x, core = tp // 2, tp % 2
    s = (y + z) % 4

    def dev(yy, zz, xx, cc):
        return (zz // 4, (zz % 4) * NY + yy, xx * 2 + cc)

    y_up, y_dn = (y + 1) % NY, (y + NY - 1) % NY
    z_up, z_dn = (z + 1) % NZ, (z + NZ - 1) % NZ
    last = s // 3
    first = (4 - s) // 4

    def pick(flag, a, b):
        return flag * a + (1 - flag) * b

    nbr = (
        (
            dev(pick(last, y_up, y), pick(last, z, z_up), x, core),
            dev(pick(first, y_dn, y), pick(first, z, z_dn), x, core),
        ),
        (
            dev(pick(last, y, y_up), pick(last, z_up, z), x, core),
            dev(pick(first, y, y_dn), pick(first, z_dn, z), x, core),
        ),
    )
    partner = dev(y, z, x, 1 - core)
    right = dev(y, z, (x + 1) % NX, core)
    left = dev(y, z, (x + NX - 1) % NX, core)
    x_r, x_l, x_far = (x + 1) % NX, (x + NX - 1) % NX, (x + 2) % NX

    def piece_row(h, d, k):
        if d == 0:
            t = (k - s + 3) // 4
            dy, dz = (t, k - t) if h == 0 else (k - t, t)
            yy, zz = (y - dy + 32) % NY, (z - dz + 32) % NZ
        else:
            t = (s + k) // 4
            dy, dz = (t, k - t) if h == 0 else (k - t, t)
            yy, zz = (y + dy) % NY, (z + dz) % NZ
        return pl.multiple_of((zz * NY + yy) * ROWS + h * PIECE, PIECE)

    def remote(src, dst, send, recv, device):
        return pltpu.make_async_remote_copy(
            src_ref=src,
            dst_ref=dst,
            send_sem=send,
            recv_sem=recv,
            device_id=device,
            device_id_type=pl.DeviceIdType.MESH,
        )

    def wait_for(ref, sem):
        pltpu.make_async_copy(ref, ref, sem).wait()

    my_rows = pl.ds(pl.multiple_of((z * NY + y) * ROWS, ROWS), ROWS)
    loads = [
        pltpu.make_async_copy(packed.at[t], wall.at[t, core, my_rows], load_sem.at[t])
        for t in range(2)
    ]
    for load in loads:
        load.start()

    barrier = pltpu.get_barrier_semaphore()
    everyone = (
        dev(y_up, z, x, core),
        dev(y_dn, z, x, core),
        dev(y, z_up, x, core),
        dev(y, z_dn, x, core),
        right,
        left,
        partner,
    )
    for device in everyone:
        pl.semaphore_signal(barrier, inc=1, device_id=device, device_id_type=pl.DeviceIdType.MESH)
    pl.semaphore_wait(barrier, len(everyone))
    for load in loads:
        load.wait()

    def ring_round(R):
        t = R // NR
        r = R % NR
        rows = {(h, d): pl.ds(piece_row(h, d, r), PIECE) for h in range(2) for d in range(2)}
        for m, (lane, width) in enumerate(LANES):
            for d in range(2):
                end = 16 - d
                blocks = [wall.at[t, core, rows[h, d], pl.ds(lane, width)] for h in range(2)]

                @pl.when(jnp.logical_and(r >= 1, r <= end))
                def _():
                    for h in range(2):
                        wait_for(blocks[h], ring_recv.at[R, h, d, m])

                @pl.when(r < end)
                def _():
                    for h in range(2):
                        remote(
                            blocks[h],
                            blocks[h],
                            ring_send.at[t, h, d],
                            ring_recv.at[R + 1, h, d, m],
                            nbr[h][d],
                        ).start()

        for d in range(2):

            @pl.when(jnp.logical_and(r >= d, r <= 16 - d))
            def _():
                for h in range(2):
                    block = wall.at[t, core, rows[h, d]]
                    remote(block, block, d2d_send.at[t], d2d_recv.at[t], partner).start()

    serves = core == y // 2
    dist = ((x - z_lo + NX) % NX, (z_lo - x + NX) % NX)
    side = (right, left)

    def cut(R):
        t = R // NR
        r = R % NR
        for d in range(2):

            @pl.when(jnp.logical_and(r >= d, r <= 16 - d))
            def _():
                for h in range(2):
                    row = piece_row(h, d, r)
                    for m, lane in enumerate((0, 640, 1408)):
                        window = wall[t, core, pl.ds(row, PIECE), lane : lane + 768]
                        window = window.astype(jnp.float32)
                        start = (64 if m == 1 else 0) + BLK * (y % 2)
                        block = pltpu.roll(window, (768 - start) % 768, 1)[:, :PAD]
                        stage[R % 2, h, d, :, m * PAD : (m + 1) * PAD] = block.astype(jnp.bfloat16)
                    pltpu.make_async_copy(
                        stage.at[R % 2, h, d],
                        served.at[t, pl.ds(row, PIECE)],
                        srecv.at[R, h, d],
                    ).start()

    def pass_on(R):
        for h in range(2):
            was = R - 2 * dist[h] - 1

            @pl.when(jnp.logical_and(was >= 0, was < 2 * NR))
            def _():
                t = was // NR
                r = was % NR
                for d in range(2):

                    @pl.when(jnp.logical_and(r >= d, r <= 16 - d))
                    def _():
                        block = served.at[t, pl.ds(piece_row(h, d, r), PIECE)]
                        wait_for(block, srecv.at[was, h, d])

                        @pl.when(dist[h] < 3)
                        def _():
                            remote(
                                block, block, s_fwd_send.at[h], srecv.at[was, h, d], side[h]
                            ).start()

                        remote(block, block, s_d2d_send, s_d2d_recv, partner).start()

    def normed(value):
        square = jnp.mean(value * value, axis=-1, keepdims=True)
        return (value * lax.rsqrt(square + EPS)).astype(jnp.bfloat16)

    halves = (pl.ds(0, HALF), pl.ds(HALF, HALF))

    def send_tokens(p):
        for i, device in enumerate((right, left)):
            for b in range(2):
                block = xa.at[p, x, halves[b]]
                remote(block, block, ag_send.at[p, i, b], ag_recv.at[p, i, b], device).start()

    def relay_tokens(p):
        for i, (device, origin) in enumerate(((right, x_l), (left, x_r))):
            block = xa.at[p, origin, halves[i]]
            wait_for(block, ag_recv.at[p, i, i])
            remote(block, block, ag_send.at[p, i, 2], ag_recv.at[p, i, 2], device).start()

    def await_tokens(p):
        for i, origin in enumerate((x_l, x_r)):
            wait_for(xa.at[p, origin, halves[1 - i]], ag_recv.at[p, i, 1 - i])
            wait_for(xa.at[p, x_far, halves[i]], ag_recv.at[p, i, 2])

    def hidden(t, c):
        tokens = xa[t].reshape(NX * TOK, D)
        pre[...] = jnp.dot(tokens, wall[t, c, :, :GU], preferred_element_type=jnp.float32)

        def rows_of(i, carry):
            rows = pl.ds(pl.multiple_of(i * HALF, HALF), HALF)
            gate = pre[rows, :DN] * IN_SCALE
            up = pltpu.roll(pre[rows, GU - DN :], DN - 64, 1) * IN_SCALE
            value = gate / (1.0 + jnp.exp(-gate)) * up
            lane = lax.broadcasted_iota(jnp.int32, value.shape, 1)
            hid[c, rows, :] = jnp.where(lane < COLS, value, 0.0).astype(jnp.bfloat16)
            return carry

        lax.fori_loop(0, NX * TOK // HALF, rows_of, 0)

    def down(t, j):
        drows = pl.ds(pl.multiple_of(j * CH, CH), CH)
        total = None
        for c in range(2):
            term = lax.dot_general(
                hid[c],
                wall[t, c, drows, GU:],
                (((1,), (1,)), ((), ())),
                preferred_element_type=jnp.float32,
            )
            total = term if total is None else total + term
        accs[...] = (total * OUT_SCALE).reshape(NX, TOK, CH)
        own[:, drows] = accs[x]
        part[0, :, drows] = accs[x_r]
        part[1, :, drows] = accs[x_l]
        st2[t, :, drows] = accs[x_far].astype(jnp.bfloat16)
        for i, device in enumerate((right, left)):
            remote(
                st2.at[t, halves[i], drows],
                cbuf.at[t, i, :, drows],
                c_send.at[t, i, j],
                c_recv.at[t, i, j],
                device,
            ).start()

    def combine(t, j):
        drows = pl.ds(pl.multiple_of(j * CH, CH), CH)
        for i, device in enumerate((right, left)):
            wait_for(cbuf.at[t, i, :, drows], c_recv.at[t, i, j])
            comb[t, i, halves[i], drows] = (
                part[i, halves[i], drows] + cbuf[t, i, :, drows].astype(jnp.float32)
            ).astype(jnp.bfloat16)
            comb[t, i, halves[1 - i], drows] = part[i, halves[1 - i], drows].astype(jnp.bfloat16)
            remote(
                comb.at[t, i, :, drows],
                rbuf.at[t, i, :, drows],
                r_send.at[t, i, j],
                r_recv.at[t, i, j],
                device,
            ).start()

    def finish(t):
        for j in range(NCH):
            for i in range(2):
                wait_for(rbuf.at[t, i, :, pl.ds(j * CH, CH)], r_recv.at[t, i, j])
        branch = own[...] + rbuf[t, 0].astype(jnp.float32) + rbuf[t, 1].astype(jnp.float32)
        return (resid[...] + 0.5 * branch).astype(jnp.bfloat16)

    start = prompt[...].astype(jnp.float32)
    resid[...] = start
    xa[0, x] = normed(start)

    def one_round(R, carry):
        @pl.when(R < 2 * NR)
        def _():
            ring_round(R)

        @pl.when(R == 0)
        def _():
            send_tokens(0)

        @pl.when(serves)
        def _():
            pass_on(R)

            @pl.when(jnp.logical_and(x == z_lo, R < 2 * NR))
            def _():
                cut(R)

        @pl.when(R == 3)
        def _():
            relay_tokens(0)

        @pl.when(R == NR - 1)
        def _():
            await_tokens(0)

        @pl.when(R == NR + 11)
        def _():
            relay_tokens(1)

        @pl.when(R == 2 * NR - 1)
        def _():
            await_tokens(1)

        t = (R - NR + NR) // NR - 1
        q = R % NR

        @pl.when(R >= NR)
        def _():
            @pl.when(q == 1)
            def _():
                wait_for(wall.at[t, 1 - core], d2d_recv.at[t])

            @pl.when(q < 2)
            def _():
                hidden(t, (core + q) % 2)

            @pl.when(jnp.logical_and(q >= 2, q < 2 + NCH))
            def _():
                down(t, q - 2)

            @pl.when(jnp.logical_and(q >= 4, q < 4 + NCH))
            def _():
                combine(t, q - 4)

        @pl.when(R == NR + 9)
        def _():
            middle = finish(0).astype(jnp.float32)
            resid[...] = middle
            xa[1, x] = normed(middle)
            send_tokens(1)

        @pl.when(R == 2 * NR + 9)
        def _():
            result[...] = finish(1)

        return carry

    lax.fori_loop(0, ROUNDS, one_round, 0)

    for t in range(2):
        for h in range(2):
            wait_for(wall.at[t, 0, pl.ds(0, 16 * PIECE)], ring_send.at[t, h, 0])
            wait_for(wall.at[t, 0, pl.ds(0, 15 * PIECE)], ring_send.at[t, h, 1])
        wait_for(wall.at[t, core], d2d_send.at[t])
        for i in range(2):
            for b in range(3):
                wait_for(xa.at[t, x, halves[0]], ag_send.at[t, i, b])
            for j in range(NCH):
                block = pl.ds(j * CH, CH)
                wait_for(st2.at[t, halves[i], block], c_send.at[t, i, j])
                wait_for(comb.at[t, i, :, block], r_send.at[t, i, j])

    @pl.when(serves)
    def _():
        for h in range(2):

            @pl.when(dist[h] < 3)
            def _():
                wait_for(served.at[0], s_fwd_send.at[h])

        wait_for(served, s_d2d_send)

    @pl.when(jnp.logical_not(serves))
    def _():
        wait_for(served, s_d2d_recv)


def on_device(
    prompt,
    norm_first,
    gate_first,
    up_first,
    down_first,
    norm_second,
    gate_second,
    up_second,
    down_second,
):
    def pack(gain, gate, up, down):
        gain = gain[:, None]
        zero = jnp.zeros((ROWS, PACK - 3 * COLS), jnp.float32)
        return jnp.concatenate([gain * gate, gain * up, down, zero], axis=1).astype(jnp.bfloat16)

    packed = jnp.stack(
        [
            pack(norm_first, gate_first, up_first, down_first),
            pack(norm_second, gate_second, up_second, down_second),
        ]
    )
    dma = pltpu.SemaphoreType.DMA
    bf16, f32 = jnp.bfloat16, jnp.float32
    served, result = pl.pallas_call(
        kernel,
        out_shape=(
            jax.ShapeDtypeStruct((2, D, SERVED), bf16),
            jax.ShapeDtypeStruct((TOK, D), bf16),
        ),
        in_specs=[
            pl.BlockSpec(memory_space=pl.ANY),
            pl.BlockSpec(memory_space=pltpu.VMEM),
        ],
        out_specs=(
            pl.BlockSpec(memory_space=pl.ANY),
            pl.BlockSpec(memory_space=pltpu.VMEM),
        ),
        scratch_shapes=[
            pltpu.VMEM((2, 2, D, PACK), bf16),
            pltpu.VMEM((2, NX, TOK, D), bf16),
            pltpu.VMEM((NX * TOK, GU), f32),
            pltpu.VMEM((2, NX * TOK, DN), bf16),
            pltpu.VMEM((NX, TOK, CH), f32),
            pltpu.VMEM((TOK, D), f32),
            pltpu.VMEM((2, TOK, D), f32),
            pltpu.VMEM((2, TOK, D), bf16),
            pltpu.VMEM((2, 2, TOK, D), bf16),
            pltpu.VMEM((2, 2, HALF, D), bf16),
            pltpu.VMEM((2, 2, TOK, D), bf16),
            pltpu.VMEM((TOK, D), f32),
            pltpu.VMEM((2, 2, 2, PIECE, SERVED), bf16),
            dma((2,)),
            dma((2 * NR, 2, 2, 3)),
            dma((2, 2, 2)),
            dma((2,)),
            dma((2,)),
            dma((2 * NR, 2, 2)),
            dma((2,)),
            dma,
            dma,
            dma((2, 2, 3)),
            dma((2, 2, 3)),
            dma((2, 2, NCH)),
            dma((2, 2, NCH)),
            dma((2, 2, NCH)),
            dma((2, 2, NCH)),
        ],
        compiler_params=pltpu.CompilerParams(
            collective_id=0, has_side_effects=True, vmem_limit_bytes=66 * 1024 * 1000
        ),
    )(packed, prompt)
    blocks = [served[t, :, m * PAD : m * PAD + BLK] for t in range(2) for m in range(3)]
    return (*blocks, result)


def solution(mesh):
    row = P(("gr", "fs"))
    tile = P(("gr", "fs"), "tp")
    token = P(("gr", "fs", "tp"), None)
    block = P(None, "fs")
    return jax.shard_map(
        on_device,
        mesh=mesh,
        in_specs=(token, row, tile, tile, tile, row, tile, tile, tile),
        out_specs=(block,) * 6 + (token,),
        check_vma=False,
    )
```

```python
import jax
import jax.numpy as jnp
from jax import lax
from jax.experimental import pallas as pl
from jax.experimental.pallas import tpu as pltpu
from jax.sharding import PartitionSpec as P

D = 2048
FF = 5632
EPS = 1e-06
NY, NZ, NX = 4, 8, 4
TOK = 96
HALF = 48
ROWS = 64
PIECE = 32
COLS = 704
BLK = 352
PACK = 2176
GU = 1408
DN = 768
YP = (0, 896)
ZQ = (896, 1280)
GROUP = NY * ROWS
CH = 512
NCH = D // CH
IN_SCALE = D ** (-0.5)
OUT_SCALE = FF ** (-0.5)


def kernel(
    packed,
    prompt,
    served,
    result,
    wall,
    xa,
    pre,
    hid,
    accs,
    own,
    part,
    st2,
    comb,
    cbuf,
    rbuf,
    resid,
    stage,
    picks,
    load_sem,
    yp_recv,
    yp_send,
    zq_recv,
    zq_send,
    zp_recv,
    zp_send,
    yq_recv,
    yq_send,
    d2d_recv,
    d2d_send,
    srecv,
    s_fwd_send,
    s_d2d_send,
    s_d2d_recv,
    ag_recv,
    ag_send,
    c_recv,
    c_send,
    r_recv,
    r_send,
):
    gr = lax.axis_index("gr")
    fs = lax.axis_index("fs")
    tp = lax.axis_index("tp")
    z_lo, y = fs // NY, fs % NY
    z = gr * 4 + z_lo
    x, core = tp // 2, tp % 2

    def dev(yy, zz, xx, cc):
        return (zz // 4, (zz % 4) * NY + yy, xx * 2 + cc)

    y_up, y_dn = (y + 1) % NY, (y + NY - 1) % NY
    z_up, z_dn = (z + 1) % NZ, (z + NZ - 1) % NZ
    along_y = (dev(y_up, z, x, core), dev(y_dn, z, x, core))
    along_z = (dev(y, z_up, x, core), dev(y, z_dn, x, core))
    partner = dev(y, z, x, 1 - core)
    right = dev(y, z, (x + 1) % NX, core)
    left = dev(y, z, (x + NX - 1) % NX, core)
    x_r, x_l, x_far = (x + 1) % NX, (x + NX - 1) % NX, (x + 2) % NX

    near_y = (y, y_dn, y_up, (y + 2) % NY)

    def from_z(d, k):
        return (z + NZ - k) % NZ if d == 0 else (z + k) % NZ

    def group_z(g):
        return (z + NZ + (1 - 2 * (g % 2)) * ((g + 1) // 2)) % NZ

    def piece(t, yy, zz, lanes, half=None):
        row = (zz * NY + yy) * ROWS
        if half is None:
            rows = pl.ds(pl.multiple_of(row, ROWS), ROWS)
        else:
            rows = pl.ds(pl.multiple_of(row + half * PIECE, PIECE), PIECE)
        return wall.at[t, core, rows, pl.ds(*lanes)]

    def remote(src, dst, send, recv, device):
        return pltpu.make_async_remote_copy(
            src_ref=src,
            dst_ref=dst,
            send_sem=send,
            recv_sem=recv,
            device_id=device,
            device_id_type=pl.DeviceIdType.MESH,
        )

    def wait_for(ref, sem):
        pltpu.make_async_copy(ref, ref, sem).wait()

    my_rows = pl.ds(pl.multiple_of((z * NY + y) * ROWS, ROWS), ROWS)
    loads = [
        pltpu.make_async_copy(packed.at[t], wall.at[t, core, my_rows], load_sem.at[t])
        for t in range(2)
    ]
    for load in loads:
        load.start()

    barrier = pltpu.get_barrier_semaphore()
    everyone = (*along_y, *along_z, right, left, partner)
    for device in everyone:
        pl.semaphore_signal(barrier, inc=1, device_id=device, device_id_type=pl.DeviceIdType.MESH)
    pl.semaphore_wait(barrier, len(everyone))
    for load in loads:
        load.wait()

    def push(block, send, recv, device):
        remote(block, block, send, recv, device).start()

    def send_zp(t, k, i, origin_z):
        half = k == 4
        for d in range(2):
            block = piece(t, near_y[i], origin_z[d], YP, d if half else None)
            push(block, zp_send.at[t, d], zp_recv.at[t, d, k - 1, i], along_z[d])

    def send_yq(t, g):
        for d in range(2):
            block = piece(t, y, group_z(g), ZQ)
            push(block, yq_send.at[t, d], yq_recv.at[t, d, g, 0], along_y[d])

    def begin(t):
        for d in range(2):
            push(piece(t, y, z, YP), yp_send.at[t, d], yp_recv.at[t, d, 0], along_y[d])
            push(piece(t, y, z, ZQ), zq_send.at[t, d], zq_recv.at[t, d, 0], along_z[d])
        send_zp(t, 1, 0, (z, z))
        send_yq(t, 0)

    def yp(t):
        for d in range(2):
            wait_for(piece(t, near_y[1 + d], z, YP), yp_recv.at[t, d, 0])
            push(piece(t, near_y[1 + d], z, YP, d), yp_send.at[t, d], yp_recv.at[t, d, 1], along_y[d])
        send_zp(t, 1, 1, (z, z))
        send_zp(t, 1, 2, (z, z))

    def yp_far(t):
        for d in range(2):
            wait_for(piece(t, near_y[3], z, YP, d), yp_recv.at[t, d, 1])
        send_zp(t, 1, 3, (z, z))

    def zq(t, k):
        for d in range(2):
            wait_for(piece(t, y, from_z(d, k), ZQ, d if k == 4 else None), zq_recv.at[t, d, k - 1])
            if k < 4:
                block = piece(t, y, from_z(d, k), ZQ, d if k == 3 else None)
                push(block, zq_send.at[t, d], zq_recv.at[t, d, k], along_z[d])
        send_yq(t, 2 * k - 1)
        if k < 4:
            send_yq(t, 2 * k)

    def zp(t, k, i):
        for d in range(2):
            block = piece(t, near_y[i], from_z(d, k), YP, d if k == 4 else None)
            wait_for(block, zp_recv.at[t, d, k - 1, i])
        if k < 4:
            send_zp(t, k + 1, i, (from_z(0, k), from_z(1, k)))

    def yq(t, g):
        for d in range(2):
            wait_for(piece(t, near_y[1 + d], group_z(g), ZQ), yq_recv.at[t, d, g, 0])
            block = piece(t, near_y[1 + d], group_z(g), ZQ, d)
            push(block, yq_send.at[t, d], yq_recv.at[t, d, g, 1], along_y[d])

    serves = core == y // 2
    dist = ((x - z_lo + NX) % NX, (z_lo - x + NX) % NX)
    side = (right, left)

    def served_part(t, g, h):
        lane = group_z(g) * GROUP + h * 128
        return served.at[t, :, :, pl.ds(pl.multiple_of(lane, 128), 128)]

    def make_picks():
        for i in range(2):
            unit = lax.broadcasted_iota(jnp.int32, (BLK, DN), 0)
            lane = lax.broadcasted_iota(jnp.int32, (BLK, DN), 1)
            wanted = unit + (BLK * (y % 2) + 64 * i)
            picks[i] = jnp.where(lane == wanted, 1.0, 0.0).astype(jnp.bfloat16)

    def cut(t, g):
        rows = pl.ds(pl.multiple_of(group_z(g) * GROUP, GROUP), GROUP)
        slot = g % 2
        for m, lane in enumerate((0, 640, 1408)):
            block = lax.dot_general(
                picks[m % 2],
                wall[t, core, rows, lane : lane + DN],
                (((1,), (1,)), ((), ())),
                preferred_element_type=jnp.float32,
            ).astype(jnp.bfloat16)
            for h in range(2):
                stage[slot, h, m] = block[:, h * 128 : (h + 1) * 128]
        for h in range(2):
            pltpu.make_async_copy(
                stage.at[slot, h], served_part(t, g, h), srecv.at[t * NZ + g, h]
            ).start()

    def pass_on(now):
        @pl.when(serves)
        def _():
            for h in range(2):
                was = now - 2 * dist[h] - 1

                @pl.when(jnp.logical_and(was >= 0, was < 2 * NZ))
                def _():
                    block = served_part(was // NZ, was % NZ, h)
                    wait_for(block, srecv.at[was, h])

                    @pl.when(dist[h] < 3)
                    def _():
                        push(block, s_fwd_send.at[h], srecv.at[was, h], side[h])

                    push(block, s_d2d_send, s_d2d_recv, partner)

    def whole(t, g):
        for d in range(2):
            wait_for(piece(t, near_y[3], group_z(g), ZQ, d), yq_recv.at[t, d, g, 1])
        rows = pl.ds(pl.multiple_of(group_z(g) * GROUP, GROUP), GROUP)
        push(wall.at[t, core, rows], d2d_send.at[t], d2d_recv.at[t], partner)
        pass_on(t * NZ + g)

        @pl.when(jnp.logical_and(serves, x == z_lo))
        def _():
            cut(t, g)

    def normed(value):
        square = jnp.mean(value * value, axis=-1, keepdims=True)
        return (value * lax.rsqrt(square + EPS)).astype(jnp.bfloat16)

    halves = (pl.ds(0, HALF), pl.ds(HALF, HALF))

    def send_tokens(p):
        for i, device in enumerate((right, left)):
            for b in range(2):
                block = xa.at[p, x, halves[b]]
                remote(block, block, ag_send.at[p, i, b], ag_recv.at[p, i, b], device).start()

    def relay_tokens(p):
        for i, (device, origin) in enumerate(((right, x_l), (left, x_r))):
            block = xa.at[p, origin, halves[i]]
            wait_for(block, ag_recv.at[p, i, i])
            remote(block, block, ag_send.at[p, i, 2], ag_recv.at[p, i, 2], device).start()

    def await_tokens(p):
        for i, origin in enumerate((x_l, x_r)):
            wait_for(xa.at[p, origin, halves[1 - i]], ag_recv.at[p, i, 1 - i])
            wait_for(xa.at[p, x_far, halves[i]], ag_recv.at[p, i, 2])

    def hidden(t, c):
        tokens = xa[t].reshape(NX * TOK, D)
        pre[...] = jnp.dot(tokens, wall[t, c, :, :GU], preferred_element_type=jnp.float32)

        def rows_of(i, carry):
            rows = pl.ds(pl.multiple_of(i * HALF, HALF), HALF)
            gate = pre[rows, :DN] * IN_SCALE
            up = pltpu.roll(pre[rows, GU - DN :], DN - 64, 1) * IN_SCALE
            value = gate / (1.0 + jnp.exp(-gate)) * up
            lane = lax.broadcasted_iota(jnp.int32, value.shape, 1)
            hid[c, rows, :] = jnp.where(lane < COLS, value, 0.0).astype(jnp.bfloat16)
            return carry

        lax.fori_loop(0, NX * TOK // HALF, rows_of, 0)

    def down(t, j):
        drows = pl.ds(pl.multiple_of(j * CH, CH), CH)
        total = None
        for c in range(2):
            term = lax.dot_general(
                hid[c],
                wall[t, c, drows, GU:],
                (((1,), (1,)), ((), ())),
                preferred_element_type=jnp.float32,
            )
            total = term if total is None else total + term
        accs[...] = (total * OUT_SCALE).reshape(NX, TOK, CH)
        own[:, drows] = accs[x]
        part[0, :, drows] = accs[x_r]
        part[1, :, drows] = accs[x_l]
        st2[t, :, drows] = accs[x_far].astype(jnp.bfloat16)
        for i, device in enumerate((right, left)):
            remote(
                st2.at[t, halves[i], drows],
                cbuf.at[t, i, :, drows],
                c_send.at[t, i, j],
                c_recv.at[t, i, j],
                device,
            ).start()

    def combine(t, j):
        drows = pl.ds(pl.multiple_of(j * CH, CH), CH)
        for i, device in enumerate((right, left)):
            wait_for(cbuf.at[t, i, :, drows], c_recv.at[t, i, j])
            comb[t, i, halves[i], drows] = (
                part[i, halves[i], drows] + cbuf[t, i, :, drows].astype(jnp.float32)
            ).astype(jnp.bfloat16)
            comb[t, i, halves[1 - i], drows] = part[i, halves[1 - i], drows].astype(jnp.bfloat16)
            remote(
                comb.at[t, i, :, drows],
                rbuf.at[t, i, :, drows],
                r_send.at[t, i, j],
                r_recv.at[t, i, j],
                device,
            ).start()

    def finish(t):
        for j in range(NCH):
            for i in range(2):
                wait_for(rbuf.at[t, i, :, pl.ds(j * CH, CH)], r_recv.at[t, i, j])
        branch = own[...] + rbuf[t, 0].astype(jnp.float32) + rbuf[t, 1].astype(jnp.float32)
        return (resid[...] + 0.5 * branch).astype(jnp.bfloat16)

    start = prompt[...].astype(jnp.float32)
    resid[...] = start
    xa[0, x] = normed(start)

    begin(0)
    send_tokens(0)
    make_picks()

    def compute(t, stage_of):
        if stage_of == 0:
            hidden(t, core)
        elif stage_of == 1:
            wait_for(wall.at[t, 1 - core], d2d_recv.at[t])
            hidden(t, 1 - core)

    def to_second():
        middle = finish(0).astype(jnp.float32)
        resid[...] = middle
        xa[1, x] = normed(middle)
        send_tokens(1)

    yp(0)
    zq(0, 1)
    zp(0, 1, 0)
    yq(0, 0)
    yp_far(0)
    zp(0, 1, 1)
    zp(0, 1, 2)
    zp(0, 1, 3)
    relay_tokens(0)
    zq(0, 2)
    whole(0, 0)
    zp(0, 2, 0)
    yq(0, 1)
    yq(0, 2)
    zp(0, 2, 1)
    zp(0, 2, 2)
    zp(0, 2, 3)
    zq(0, 3)
    whole(0, 1)
    whole(0, 2)
    zp(0, 3, 0)
    yq(0, 3)
    yq(0, 4)
    zp(0, 3, 1)
    zp(0, 3, 2)
    zp(0, 3, 3)
    zq(0, 4)
    begin(1)
    whole(0, 3)
    whole(0, 4)
    zp(0, 4, 0)
    yq(0, 5)
    yq(0, 6)
    zp(0, 4, 1)
    zp(0, 4, 2)
    zp(0, 4, 3)
    yq(0, 7)
    yp(1)
    zq(1, 1)
    whole(0, 5)
    whole(0, 6)
    zp(1, 1, 0)
    whole(0, 7)
    await_tokens(0)
    yq(1, 0)
    yp_far(1)
    compute(0, 0)
    zp(1, 1, 1)
    zp(1, 1, 2)
    zp(1, 1, 3)
    zq(1, 2)
    compute(0, 1)
    whole(1, 0)
    zp(1, 2, 0)
    down(0, 0)
    yq(1, 1)
    down(0, 1)
    yq(1, 2)
    zp(1, 2, 1)
    down(0, 2)
    combine(0, 0)
    zp(1, 2, 2)
    down(0, 3)
    combine(0, 1)
    zp(1, 2, 3)
    zq(1, 3)
    combine(0, 2)
    whole(1, 1)
    combine(0, 3)
    whole(1, 2)
    zp(1, 3, 0)
    yq(1, 3)
    yq(1, 4)
    zp(1, 3, 1)
    zp(1, 3, 2)
    zp(1, 3, 3)
    to_second()
    zq(1, 4)
    whole(1, 3)
    whole(1, 4)
    zp(1, 4, 0)
    relay_tokens(1)
    yq(1, 5)
    yq(1, 6)
    zp(1, 4, 1)
    zp(1, 4, 2)
    zp(1, 4, 3)
    whole(1, 5)
    whole(1, 6)
    yq(1, 7)
    whole(1, 7)
    await_tokens(1)
    pass_on(16)
    compute(1, 0)
    pass_on(17)
    compute(1, 1)
    down(1, 0)
    pass_on(18)
    down(1, 1)
    down(1, 2)
    combine(1, 0)
    pass_on(19)
    down(1, 3)
    combine(1, 1)
    pass_on(20)
    combine(1, 2)
    pass_on(21)
    combine(1, 3)
    pass_on(22)
    result[...] = finish(1)

    def some(rows, lanes):
        return wall.at[0, 0, pl.ds(0, rows), pl.ds(*lanes)]

    for t in range(2):
        for d in range(2):
            wait_for(some(96, YP), yp_send.at[t, d])
            wait_for(some(NZ * 96, ZQ), yq_send.at[t, d])
            wait_for(some(224, ZQ), zq_send.at[t, d])
            wait_for(some(NY * 224, YP), zp_send.at[t, d])
        wait_for(wall.at[t, core], d2d_send.at[t])
        for i in range(2):
            for b in range(3):
                wait_for(xa.at[t, x, halves[0]], ag_send.at[t, i, b])
            for j in range(NCH):
                block = pl.ds(j * CH, CH)
                wait_for(st2.at[t, halves[i], block], c_send.at[t, i, j])
                wait_for(comb.at[t, i, :, block], r_send.at[t, i, j])

    @pl.when(serves)
    def _():
        for h in range(2):

            @pl.when(dist[h] < 3)
            def _():
                wait_for(served.at[0], s_fwd_send.at[h])

        wait_for(served, s_d2d_send)

    @pl.when(jnp.logical_not(serves))
    def _():
        wait_for(served, s_d2d_recv)


def on_device(
    prompt,
    norm_first,
    gate_first,
    up_first,
    down_first,
    norm_second,
    gate_second,
    up_second,
    down_second,
):
    def pack(gain, gate, up, down):
        gain = gain[:, None]
        zero = jnp.zeros((ROWS, PACK - 3 * COLS), jnp.float32)
        return jnp.concatenate([gain * gate, gain * up, down, zero], axis=1).astype(jnp.bfloat16)

    packed = jnp.stack(
        [
            pack(norm_first, gate_first, up_first, down_first),
            pack(norm_second, gate_second, up_second, down_second),
        ]
    )
    dma = pltpu.SemaphoreType.DMA
    bf16, f32 = jnp.bfloat16, jnp.float32
    served, result = pl.pallas_call(
        kernel,
        out_shape=(
            jax.ShapeDtypeStruct((2, 3, BLK, D), bf16),
            jax.ShapeDtypeStruct((TOK, D), bf16),
        ),
        in_specs=[
            pl.BlockSpec(memory_space=pl.ANY),
            pl.BlockSpec(memory_space=pltpu.VMEM),
        ],
        out_specs=(
            pl.BlockSpec(memory_space=pl.ANY),
            pl.BlockSpec(memory_space=pltpu.VMEM),
        ),
        scratch_shapes=[
            pltpu.VMEM((2, 2, D, PACK), bf16),
            pltpu.VMEM((2, NX, TOK, D), bf16),
            pltpu.VMEM((NX * TOK, GU), f32),
            pltpu.VMEM((2, NX * TOK, DN), bf16),
            pltpu.VMEM((NX, TOK, CH), f32),
            pltpu.VMEM((TOK, D), f32),
            pltpu.VMEM((2, TOK, D), f32),
            pltpu.VMEM((2, TOK, D), bf16),
            pltpu.VMEM((2, 2, TOK, D), bf16),
            pltpu.VMEM((2, 2, HALF, D), bf16),
            pltpu.VMEM((2, 2, TOK, D), bf16),
            pltpu.VMEM((TOK, D), f32),
            pltpu.VMEM((2, 2, 3, BLK, 128), bf16),
            pltpu.VMEM((2, BLK, DN), bf16),
            dma((2,)),
            dma((2, 2, 2)),
            dma((2, 2)),
            dma((2, 2, 4)),
            dma((2, 2)),
            dma((2, 2, 4, NY)),
            dma((2, 2)),
            dma((2, 2, NZ, 2)),
            dma((2, 2)),
            dma((2,)),
            dma((2,)),
            dma((2 * NZ, 2)),
            dma((2,)),
            dma,
            dma,
            dma((2, 2, 3)),
            dma((2, 2, 3)),
            dma((2, 2, NCH)),
            dma((2, 2, NCH)),
            dma((2, 2, NCH)),
            dma((2, 2, NCH)),
        ],
        compiler_params=pltpu.CompilerParams(
            collective_id=0, has_side_effects=True, vmem_limit_bytes=66 * 1024 * 1000
        ),
    )(packed, prompt)
    blocks = [served[t, m].T for t in range(2) for m in range(3)]
    return (*blocks, result)


def solution(mesh):
    row = P(("gr", "fs"))
    tile = P(("gr", "fs"), "tp")
    token = P(("gr", "fs", "tp"), None)
    block = P(None, "fs")
    return jax.shard_map(
        on_device,
        mesh=mesh,
        in_specs=(token, row, tile, tile, tile, row, tile, tile, tile),
        out_specs=(block,) * 6 + (token,),
        check_vma=False,
    )
```

```python
import jax
import jax.numpy as jnp
from jax import lax
from jax.experimental import pallas as pl
from jax.experimental.pallas import tpu as pltpu
from jax.sharding import PartitionSpec as P

D = 2048
FF = 5632
EPS = 1e-06
NY, NZ, NX = 4, 8, 4
TOK = 96
HALF = 48
ROWS = 64
PIECE = 32
COLS = 704
BLK = 352
PACK = 2176
GU = 1408
DN = 768
YP = ((0, 640), (1408, 256))
ZQ = ((640, 768), (1664, 512))
ALL = ((0, 1408), (1408, 768))
STREAMS = 4
GROUP = NY * ROWS
CH = GROUP
NCH = NZ
IN_SCALE = D ** (-0.5)
OUT_SCALE = FF ** (-0.5)


STARTS = (0.0, 18.0, 46.0, 66.0)
PACES = (10.5, 9.5, 11.0, 9.5)


def plan():
    steps = []

    def at(time, name, *args):
        steps.append((time, name, args))

    at(STARTS[0] - 0.3, "send_tokens", 0)
    at(STARTS[0] - 0.2, "make_picks")
    at(9.0, "relay_tokens", 0)
    ready = {}
    for t, (b, pace) in enumerate(zip(STARTS, PACES)):
        at(b - 0.5, "begin", t)
        at(b + 5.5, "yp", t)
        at(b + 9.8, "yp_far", t)
        at(b + 7.0 + 0.3 * pace, "yq", t, 0)
        for k in range(1, 5):
            base = b + 7.0 + (k - 1) * pace
            at(base, "zq", t, k)
            for i in range(4):
                at(base + pace * (0.2 + i * 0.18) + (0.1 if k == 1 else 0.0), "zp", t, k, i)
            if k < 4:
                at(base + pace * 0.84, "yq", t, 2 * k - 1)
                at(base + pace * 0.92, "yq", t, 2 * k)
            else:
                at(base + pace * 0.76, "yq", t, 7)
        done = [b + 7.0 + pace]
        for k in range(1, 4):
            done += [b + 7.0 + pace * (k + 0.5) + 0.8 * w for w in range(2)]
        done.append(b + 7.0 + 4 * pace)
        for g in range(NZ):
            at(done[g], "whole", t, g)
            ready[t, g] = done[g]
            for d in range(4):
                hops = 1 if t == STREAMS - 1 and d == 3 else d
                lag = 1.5 + hops * (6.5 if t % 2 == 0 else 5.5)
                at(done[g] + lag, "pass_on", t * NZ + g, d)
    for t in range(2):
        go = ready[2 * t, 7] + 0.3
        at(go, "await_tokens", t)
        at(go + 0.1, "compute", t, 0)
        at(go + 4.5, "compute", t, 1)
        then = go + 8.0
        for g in range(NZ):
            then = max(then + 0.9, ready[2 * t + 1, g] + 2.5)
            at(then, "down", t, g)
            at(then + 5.5, "combine", t, g)
        if t == 0:
            at(then + 14.0, "to_second")
            at(then + 22.0, "relay_tokens", 1)
        else:
            at(then + 12.0, "last_step")
    return sorted(steps, key=lambda step: step[0])


def kernel(
    packed,
    prompt,
    served,
    result,
    wall,
    xa,
    pre,
    hid,
    accs,
    own,
    part,
    st2,
    comb,
    cbuf,
    rbuf,
    resid,
    stage,
    picks,
    load_sem,
    yp_recv,
    yp_send,
    zq_recv,
    zq_send,
    zp_recv,
    zp_send,
    yq_recv,
    yq_send,
    d2d_recv,
    d2d_send,
    srecv,
    s_fwd_send,
    s_last_send,
    s_d2d_send,
    s_d2d_recv,
    ag_recv,
    ag_send,
    c_recv,
    c_send,
    r_recv,
    r_send,
):
    gr = lax.axis_index("gr")
    fs = lax.axis_index("fs")
    tp = lax.axis_index("tp")
    z_lo, y = fs // NY, fs % NY
    z = gr * 4 + z_lo
    x, core = tp // 2, tp % 2

    def dev(yy, zz, xx, cc):
        return (zz // 4, (zz % 4) * NY + yy, xx * 2 + cc)

    y_up, y_dn = (y + 1) % NY, (y + NY - 1) % NY
    z_up, z_dn = (z + 1) % NZ, (z + NZ - 1) % NZ
    along_y = (dev(y_up, z, x, core), dev(y_dn, z, x, core))
    along_z = (dev(y, z_up, x, core), dev(y, z_dn, x, core))
    partner = dev(y, z, x, 1 - core)
    right = dev(y, z, (x + 1) % NX, core)
    left = dev(y, z, (x + NX - 1) % NX, core)
    x_r, x_l, x_far = (x + 1) % NX, (x + NX - 1) % NX, (x + 2) % NX

    near_y = (y, y_dn, y_up, (y + 2) % NY)

    def from_z(d, k):
        return (z + NZ - k) % NZ if d == 0 else (z + k) % NZ

    def group_z(g):
        return (z + NZ + (1 - 2 * (g % 2)) * ((g + 1) // 2)) % NZ

    def piece(t, yy, zz, lanes, half=None):
        lanes = lanes[t % 2]
        row = (zz * NY + yy) * ROWS
        if half is None:
            rows = pl.ds(pl.multiple_of(row, ROWS), ROWS)
        else:
            rows = pl.ds(pl.multiple_of(row + half * PIECE, PIECE), PIECE)
        return wall.at[t // 2, core, rows, pl.ds(*lanes)]

    def remote(src, dst, send, recv, device):
        return pltpu.make_async_remote_copy(
            src_ref=src,
            dst_ref=dst,
            send_sem=send,
            recv_sem=recv,
            device_id=device,
            device_id_type=pl.DeviceIdType.MESH,
        )

    def wait_for(ref, sem):
        pltpu.make_async_copy(ref, ref, sem).wait()

    my_rows = pl.ds(pl.multiple_of((z * NY + y) * ROWS, ROWS), ROWS)
    loads = [
        pltpu.make_async_copy(packed.at[t], wall.at[t, core, my_rows], load_sem.at[t])
        for t in range(2)
    ]
    for load in loads:
        load.start()

    barrier = pltpu.get_barrier_semaphore()
    everyone = (*along_y, *along_z, right, left, partner)
    for device in everyone:
        pl.semaphore_signal(barrier, inc=1, device_id=device, device_id_type=pl.DeviceIdType.MESH)
    pl.semaphore_wait(barrier, len(everyone))
    for load in loads:
        load.wait()

    def push(block, send, recv, device):
        remote(block, block, send, recv, device).start()

    def send_zp(t, k, i, origin_z):
        half = k == 4
        for d in range(2):
            block = piece(t, near_y[i], origin_z[d], YP, d if half else None)
            push(block, zp_send.at[t, d], zp_recv.at[t, d, k - 1, i], along_z[d])

    def send_yq(t, g):
        for d in range(2):
            block = piece(t, y, group_z(g), ZQ)
            push(block, yq_send.at[t, d], yq_recv.at[t, d, g, 0], along_y[d])

    def begin(t):
        for d in range(2):
            push(piece(t, y, z, YP), yp_send.at[t, d], yp_recv.at[t, d, 0], along_y[d])
            push(piece(t, y, z, ZQ), zq_send.at[t, d], zq_recv.at[t, d, 0], along_z[d])
        send_zp(t, 1, 0, (z, z))
        send_yq(t, 0)

    def yp(t):
        for d in range(2):
            wait_for(piece(t, near_y[1 + d], z, YP), yp_recv.at[t, d, 0])
            push(piece(t, near_y[1 + d], z, YP, d), yp_send.at[t, d], yp_recv.at[t, d, 1], along_y[d])
        send_zp(t, 1, 1, (z, z))
        send_zp(t, 1, 2, (z, z))

    def yp_far(t):
        for d in range(2):
            wait_for(piece(t, near_y[3], z, YP, d), yp_recv.at[t, d, 1])
        send_zp(t, 1, 3, (z, z))

    def zq(t, k):
        for d in range(2):
            wait_for(piece(t, y, from_z(d, k), ZQ, d if k == 4 else None), zq_recv.at[t, d, k - 1])
            if k < 4:
                block = piece(t, y, from_z(d, k), ZQ, d if k == 3 else None)
                push(block, zq_send.at[t, d], zq_recv.at[t, d, k], along_z[d])
        send_yq(t, 2 * k - 1)
        if k < 4:
            send_yq(t, 2 * k)

    def zp(t, k, i):
        for d in range(2):
            block = piece(t, near_y[i], from_z(d, k), YP, d if k == 4 else None)
            wait_for(block, zp_recv.at[t, d, k - 1, i])
        if k < 4:
            send_zp(t, k + 1, i, (from_z(0, k), from_z(1, k)))

    def yq(t, g):
        for d in range(2):
            wait_for(piece(t, near_y[1 + d], group_z(g), ZQ), yq_recv.at[t, d, g, 0])
            block = piece(t, near_y[1 + d], group_z(g), ZQ, d)
            push(block, yq_send.at[t, d], yq_recv.at[t, d, g, 1], along_y[d])

    serves = core == y // 2
    dist = ((x - z_lo + NX) % NX, (z_lo - x + NX) % NX)
    side = (right, left)

    def served_part(t, kind, g, h):
        lane = pl.multiple_of(group_z(g) * GROUP + h * 128, 128)
        which = pl.ds(2, 1) if kind else pl.ds(0, 2)
        return served.at[t, which, :, pl.ds(lane, 128)]

    def make_picks():
        for i in range(2):
            unit = lax.broadcasted_iota(jnp.int32, (BLK, DN), 0)
            lane = lax.broadcasted_iota(jnp.int32, (BLK, DN), 1)
            wanted = unit + (BLK * (y % 2) + 64 * i)
            picks[i] = jnp.where(lane == wanted, 1.0, 0.0).astype(jnp.bfloat16)

    def cut(t, g):
        rows = pl.ds(pl.multiple_of(group_z(g) * GROUP, GROUP), GROUP)
        slot = g % 2
        kind = t % 2
        for m, lane in ((2, GU),) if kind else ((0, 0), (1, 640)):
            block = lax.dot_general(
                picks[m % 2],
                wall[t // 2, core, rows, lane : lane + DN],
                (((1,), (1,)), ((), ())),
                preferred_element_type=jnp.float32,
            ).astype(jnp.bfloat16)
            for h in range(2):
                stage[slot, h, m] = block[:, h * 128 : (h + 1) * 128]
        for h in range(2):
            src = stage.at[slot, h, pl.ds(2, 1) if kind else pl.ds(0, 2)]
            pltpu.make_async_copy(
                src, served_part(t // 2, kind, g, h), srecv.at[t * NZ + g, h]
            ).start()

    def pass_on(e, d):
        t, g = e // NZ, e % NZ

        @pl.when(serves)
        def _():
            for h in range(2):

                @pl.when(dist[h] == d)
                def _():
                    block = served_part(t // 2, t % 2, g, h)
                    wait_for(block, srecv.at[e, h])
                    if t < STREAMS - 1:
                        if d < 3:
                            push(block, s_fwd_send.at[t // 2, h], srecv.at[e, h], side[h])
                    elif d == 0:
                        for device in side:
                            push(block, s_last_send.at[h], srecv.at[e, h], device)
                    elif d == 1:
                        push(block, s_last_send.at[h], srecv.at[e, h], side[h])
                    push(block, s_d2d_send, s_d2d_recv, partner)

    def whole(t, g):
        for d in range(2):
            wait_for(piece(t, near_y[3], group_z(g), ZQ, d), yq_recv.at[t, d, g, 1])
        rows = pl.ds(pl.multiple_of(group_z(g) * GROUP, GROUP), GROUP)
        block = wall.at[t // 2, core, rows, pl.ds(*ALL[t % 2])]
        landed = d2d_recv.at[t // 2, g if t % 2 else NZ]
        push(block, d2d_send.at[t], landed, partner)

        @pl.when(jnp.logical_and(serves, x == z_lo))
        def _():
            cut(t, g)

    def normed(value):
        square = jnp.mean(value * value, axis=-1, keepdims=True)
        return (value * lax.rsqrt(square + EPS)).astype(jnp.bfloat16)

    halves = (pl.ds(0, HALF), pl.ds(HALF, HALF))

    def send_tokens(p):
        for i, device in enumerate((right, left)):
            for b in range(2):
                block = xa.at[p, x, halves[b]]
                remote(block, block, ag_send.at[p, i, b], ag_recv.at[p, i, b], device).start()

    def relay_tokens(p):
        for i, (device, origin) in enumerate(((right, x_l), (left, x_r))):
            block = xa.at[p, origin, halves[i]]
            wait_for(block, ag_recv.at[p, i, i])
            remote(block, block, ag_send.at[p, i, 2], ag_recv.at[p, i, 2], device).start()

    def await_tokens(p):
        for i, origin in enumerate((x_l, x_r)):
            wait_for(xa.at[p, origin, halves[1 - i]], ag_recv.at[p, i, 1 - i])
            wait_for(xa.at[p, x_far, halves[i]], ag_recv.at[p, i, 2])

    def hidden(t, c):
        tokens = xa[t].reshape(NX * TOK, D)
        pre[...] = jnp.dot(tokens, wall[t, c, :, :GU], preferred_element_type=jnp.float32)

        def rows_of(i, carry):
            rows = pl.ds(pl.multiple_of(i * HALF, HALF), HALF)
            gate = pre[rows, :DN] * IN_SCALE
            up = pltpu.roll(pre[rows, GU - DN :], DN - 64, 1) * IN_SCALE
            value = gate / (1.0 + jnp.exp(-gate)) * up
            lane = lax.broadcasted_iota(jnp.int32, value.shape, 1)
            hid[c, rows, :] = jnp.where(lane < COLS, value, 0.0).astype(jnp.bfloat16)
            return carry

        lax.fori_loop(0, NX * TOK // HALF, rows_of, 0)

    def columns(g):
        return pl.ds(pl.multiple_of(group_z(g) * CH, CH), CH)

    def down(t, j):
        drows = columns(j)
        wait_for(wall.at[t, 1 - core, drows, pl.ds(*ALL[1])], d2d_recv.at[t, j])
        total = None
        for c in range(2):
            term = lax.dot_general(
                hid[c],
                wall[t, c, drows, GU:],
                (((1,), (1,)), ((), ())),
                preferred_element_type=jnp.float32,
            )
            total = term if total is None else total + term
        accs[...] = (total * OUT_SCALE).reshape(NX, TOK, CH)
        own[:, drows] = accs[x]
        part[0, :, drows] = accs[x_r]
        part[1, :, drows] = accs[x_l]
        st2[t, :, drows] = accs[x_far].astype(jnp.bfloat16)
        for i, device in enumerate((right, left)):
            remote(
                st2.at[t, halves[i], drows],
                cbuf.at[t, i, :, drows],
                c_send.at[t, i, j],
                c_recv.at[t, i, j],
                device,
            ).start()

    def combine(t, j):
        drows = columns(j)
        for i, device in enumerate((right, left)):
            wait_for(cbuf.at[t, i, :, drows], c_recv.at[t, i, j])
            comb[t, i, halves[i], drows] = (
                part[i, halves[i], drows] + cbuf[t, i, :, drows].astype(jnp.float32)
            ).astype(jnp.bfloat16)
            comb[t, i, halves[1 - i], drows] = part[i, halves[1 - i], drows].astype(jnp.bfloat16)
            remote(
                comb.at[t, i, :, drows],
                rbuf.at[t, i, :, drows],
                r_send.at[t, i, j],
                r_recv.at[t, i, j],
                device,
            ).start()

    def finish(t):
        for j in range(NCH):
            for i in range(2):
                wait_for(rbuf.at[t, i, :, columns(j)], r_recv.at[t, i, j])
        branch = own[...] + rbuf[t, 0].astype(jnp.float32) + rbuf[t, 1].astype(jnp.float32)
        return (resid[...] + 0.5 * branch).astype(jnp.bfloat16)

    start = prompt[...].astype(jnp.float32)
    resid[...] = start
    xa[0, x] = normed(start)

    def compute(t, stage_of):
        if stage_of == 0:
            hidden(t, core)
        elif stage_of == 1:
            wait_for(wall.at[t, 1 - core, :, pl.ds(*ALL[0])], d2d_recv.at[t, NZ])
            hidden(t, 1 - core)

    def to_second():
        middle = finish(0).astype(jnp.float32)
        resid[...] = middle
        xa[1, x] = normed(middle)
        send_tokens(1)

    def last_step():
        result[...] = finish(1)

    steps = dict(
        begin=begin,
        yp=yp,
        yp_far=yp_far,
        zq=zq,
        zp=zp,
        yq=yq,
        whole=whole,
        pass_on=pass_on,
        send_tokens=send_tokens,
        relay_tokens=relay_tokens,
        await_tokens=await_tokens,
        make_picks=make_picks,
        compute=compute,
        down=down,
        combine=combine,
        to_second=to_second,
        last_step=last_step,
    )
    for _, name, args in plan():
        steps[name](*args)

    def some(rows, lanes):
        return wall.at[0, 0, pl.ds(0, rows), pl.ds(*lanes)]

    for t in range(STREAMS):
        p_lanes, q_lanes = YP[t % 2], ZQ[t % 2]
        for d in range(2):
            wait_for(some(96, p_lanes), yp_send.at[t, d])
            wait_for(some(NZ * 96, q_lanes), yq_send.at[t, d])
            wait_for(some(224, q_lanes), zq_send.at[t, d])
            wait_for(some(NY * 224, p_lanes), zp_send.at[t, d])
        wait_for(some(D, ALL[t % 2]), d2d_send.at[t])
    for t in range(2):
        for i in range(2):
            for b in range(3):
                wait_for(xa.at[t, x, halves[0]], ag_send.at[t, i, b])
            for j in range(NCH):
                block = pl.ds(j * CH, CH)
                wait_for(st2.at[t, halves[i], block], c_send.at[t, i, j])
                wait_for(comb.at[t, i, :, block], r_send.at[t, i, j])

    @pl.when(serves)
    def _():
        for h in range(2):

            half = pl.ds(0, D // 2)

            @pl.when(dist[h] < 3)
            def _():
                wait_for(served.at[0, :, :, half], s_fwd_send.at[0, h])
                wait_for(served.at[0, pl.ds(0, 2), :, half], s_fwd_send.at[1, h])

            for d, sends in ((0, 2), (1, 1)):

                @pl.when(dist[h] == d)
                def _():
                    wait_for(served.at[0, pl.ds(0, sends), :, half], s_last_send.at[h])

        wait_for(served, s_d2d_send)

    @pl.when(jnp.logical_not(serves))
    def _():
        wait_for(served, s_d2d_recv)


def on_device(
    prompt,
    norm_first,
    gate_first,
    up_first,
    down_first,
    norm_second,
    gate_second,
    up_second,
    down_second,
):
    def pack(gain, gate, up, down):
        gain = gain[:, None]
        zero = jnp.zeros((ROWS, PACK - 3 * COLS), jnp.float32)
        return jnp.concatenate([gain * gate, gain * up, down, zero], axis=1).astype(jnp.bfloat16)

    packed = jnp.stack(
        [
            pack(norm_first, gate_first, up_first, down_first),
            pack(norm_second, gate_second, up_second, down_second),
        ]
    )
    dma = pltpu.SemaphoreType.DMA
    bf16, f32 = jnp.bfloat16, jnp.float32
    served, result = pl.pallas_call(
        kernel,
        out_shape=(
            jax.ShapeDtypeStruct((2, 3, BLK, D), bf16),
            jax.ShapeDtypeStruct((TOK, D), bf16),
        ),
        in_specs=[
            pl.BlockSpec(memory_space=pl.ANY),
            pl.BlockSpec(memory_space=pltpu.VMEM),
        ],
        out_specs=(
            pl.BlockSpec(memory_space=pl.ANY),
            pl.BlockSpec(memory_space=pltpu.VMEM),
        ),
        scratch_shapes=[
            pltpu.VMEM((2, 2, D, PACK), bf16),
            pltpu.VMEM((2, NX, TOK, D), bf16),
            pltpu.VMEM((NX * TOK, GU), f32),
            pltpu.VMEM((2, NX * TOK, DN), bf16),
            pltpu.VMEM((NX, TOK, CH), f32),
            pltpu.VMEM((TOK, D), f32),
            pltpu.VMEM((2, TOK, D), f32),
            pltpu.VMEM((2, TOK, D), bf16),
            pltpu.VMEM((2, 2, TOK, D), bf16),
            pltpu.VMEM((2, 2, HALF, D), bf16),
            pltpu.VMEM((2, 2, TOK, D), bf16),
            pltpu.VMEM((TOK, D), f32),
            pltpu.VMEM((2, 2, 3, BLK, 128), bf16),
            pltpu.VMEM((2, BLK, DN), bf16),
            dma((2,)),
            dma((STREAMS, 2, 2)),
            dma((STREAMS, 2)),
            dma((STREAMS, 2, 4)),
            dma((STREAMS, 2)),
            dma((STREAMS, 2, 4, NY)),
            dma((STREAMS, 2)),
            dma((STREAMS, 2, NZ, 2)),
            dma((STREAMS, 2)),
            dma((2, NZ + 1)),
            dma((STREAMS,)),
            dma((STREAMS * NZ, 2)),
            dma((2, 2)),
            dma((2,)),
            dma,
            dma,
            dma((2, 2, 3)),
            dma((2, 2, 3)),
            dma((2, 2, NCH)),
            dma((2, 2, NCH)),
            dma((2, 2, NCH)),
            dma((2, 2, NCH)),
        ],
        compiler_params=pltpu.CompilerParams(
            collective_id=0, has_side_effects=True, vmem_limit_bytes=66 * 1024 * 1000
        ),
    )(packed, prompt)
    blocks = [served[t, m].T for t in range(2) for m in range(3)]
    return (*blocks, result)


def solution(mesh):
    row = P(("gr", "fs"))
    tile = P(("gr", "fs"), "tp")
    token = P(("gr", "fs", "tp"), None)
    block = P(None, "fs")
    return jax.shard_map(
        on_device,
        mesh=mesh,
        in_specs=(token, row, tile, tile, tile, row, tile, tile, tile),
        out_specs=(block,) * 6 + (token,),
        check_vma=False,
    )
```

```python
import jax
import jax.numpy as jnp
from jax import lax
from jax.experimental import pallas as pl
from jax.experimental.pallas import tpu as pltpu
from jax.sharding import PartitionSpec as P

D = 2048
FF = 5632
EPS = 1e-06
NY, NZ, NX = 4, 8, 4
TOK = 96
HALF = 48
ROWS = 64
PIECE = 32
COLS = 704
BLK = 352
PACK = 2176
GU = 1408
DN = 768
YP = ((0, 640), (1408, 256))
ZQ = ((640, 768), (1664, 512))
ALL = ((0, 1408), (1408, 768))
STREAMS = 4
GROUP = NY * ROWS
CH = GROUP
NCH = NZ
IN_SCALE = D ** (-0.5)
OUT_SCALE = FF ** (-0.5)


STARTS = (0.0, 18.0, 46.0, 66.0)
PACES = (10.5, 9.5, 11.0, 9.5)


def plan():
    steps = []

    def at(time, name, *args):
        steps.append((time, name, args))

    at(STARTS[0] - 0.3, "send_tokens", 0)
    at(STARTS[0] - 0.2, "make_picks")
    at(9.0, "relay_tokens", 0)
    ready = {}
    for t, (b, pace) in enumerate(zip(STARTS, PACES)):
        at(b - 0.5, "begin", t)
        at(b + 5.5, "yp", t)
        at(b + 9.8, "yp_far", t)
        at(b + 7.0 + 0.3 * pace, "yq", t, 0)
        for k in range(1, 5):
            base = b + 7.0 + (k - 1) * pace
            at(base, "zq", t, k)
            for i in range(4):
                at(base + pace * (0.2 + i * 0.18) + (0.1 if k == 1 else 0.0), "zp", t, k, i)
            if k < 4:
                at(base + pace * 0.84, "yq", t, 2 * k - 1)
                at(base + pace * 0.92, "yq", t, 2 * k)
            else:
                at(base + pace * 0.76, "yq", t, 7)
        done = [b + 7.0 + pace]
        for k in range(1, 4):
            done += [b + 7.0 + pace * (k + 0.5) + 0.8 * w for w in range(2)]
        done.append(b + 7.0 + 4 * pace)
        for g in range(NZ):
            at(done[g], "whole", t, g)
            ready[t, g] = done[g]
            for d in range(4):
                hops = 1 if t == STREAMS - 1 and d == 3 else d
                lag = 1.5 + hops * (6.5 if t % 2 == 0 else 5.5)
                at(done[g] + lag, "pass_on", t * NZ + g, d)
    for t in range(2):
        go = ready[2 * t, 7] + 0.3
        at(go, "await_tokens", t)
        at(go + 0.1, "compute", t, 0)
        at(go + 4.5, "compute", t, 1)
        then = go + 8.0
        for g in range(NZ):
            then = max(then + 0.9, ready[2 * t + 1, g] + 2.5)
            at(then, "down", t, g)
            at(then + 5.5, "combine", t, g)
        if t == 0:
            at(then + 14.0, "to_second")
            at(then + 22.0, "relay_tokens", 1)
        else:
            at(then + 12.0, "last_step")
    return sorted(steps, key=lambda step: step[0])


def kernel(
    packed,
    prompt,
    served,
    result,
    wall,
    xa,
    pre,
    hid,
    accs,
    own,
    part,
    st2,
    comb,
    cbuf,
    rbuf,
    resid,
    stage,
    picks,
    load_sem,
    yp_recv,
    yp_send,
    zq_recv,
    zq_send,
    zp_recv,
    zp_send,
    yq_recv,
    yq_send,
    d2d_recv,
    d2d_send,
    srecv,
    s_fwd_send,
    s_last_send,
    s_d2d_send,
    s_d2d_recv,
    ag_recv,
    ag_send,
    c_recv,
    c_send,
    r_recv,
    r_send,
):
    gr = lax.axis_index("gr")
    fs = lax.axis_index("fs")
    tp = lax.axis_index("tp")
    z_lo, y = fs // NY, fs % NY
    z = gr * 4 + z_lo
    x, core = tp // 2, tp % 2

    def dev(yy, zz, xx, cc):
        return (zz // 4, (zz % 4) * NY + yy, xx * 2 + cc)

    y_up, y_dn = (y + 1) % NY, (y + NY - 1) % NY
    z_up, z_dn = (z + 1) % NZ, (z + NZ - 1) % NZ
    along_y = (dev(y_up, z, x, core), dev(y_dn, z, x, core))
    along_z = (dev(y, z_up, x, core), dev(y, z_dn, x, core))
    partner = dev(y, z, x, 1 - core)
    right = dev(y, z, (x + 1) % NX, core)
    left = dev(y, z, (x + NX - 1) % NX, core)
    x_r, x_l, x_far = (x + 1) % NX, (x + NX - 1) % NX, (x + 2) % NX

    near_y = (y, y_dn, y_up, (y + 2) % NY)

    def from_z(d, k):
        return (z + NZ - k) % NZ if d == 0 else (z + k) % NZ

    def group_z(g):
        return (z + NZ + (1 - 2 * (g % 2)) * ((g + 1) // 2)) % NZ

    def piece(t, yy, zz, lanes, half=None):
        lanes = lanes[t % 2]
        row = (zz * NY + yy) * ROWS
        if half is None:
            rows = pl.ds(pl.multiple_of(row, ROWS), ROWS)
        else:
            rows = pl.ds(pl.multiple_of(row + half * PIECE, PIECE), PIECE)
        return wall.at[t // 2, core, rows, pl.ds(*lanes)]

    def remote(src, dst, send, recv, device):
        return pltpu.make_async_remote_copy(
            src_ref=src,
            dst_ref=dst,
            send_sem=send,
            recv_sem=recv,
            device_id=device,
            device_id_type=pl.DeviceIdType.MESH,
        )

    def wait_for(ref, sem):
        pltpu.make_async_copy(ref, ref, sem).wait()

    my_rows = pl.ds(pl.multiple_of((z * NY + y) * ROWS, ROWS), ROWS)
    loads = [
        pltpu.make_async_copy(packed.at[t], wall.at[t, core, my_rows], load_sem.at[t])
        for t in range(2)
    ]
    for load in loads:
        load.start()

    barrier = pltpu.get_barrier_semaphore()
    everyone = (*along_y, *along_z, right, left, partner)
    for device in everyone:
        pl.semaphore_signal(barrier, inc=1, device_id=device, device_id_type=pl.DeviceIdType.MESH)
    pl.semaphore_wait(barrier, len(everyone))
    for load in loads:
        load.wait()

    def push(block, send, recv, device):
        remote(block, block, send, recv, device).start()

    def send_zp(t, k, i, origin_z):
        half = k == 4
        for d in range(2):
            block = piece(t, near_y[i], origin_z[d], YP, d if half else None)
            push(block, zp_send.at[t, d], zp_recv.at[t, d, k - 1, i], along_z[d])

    def send_yq(t, g):
        for d in range(2):
            block = piece(t, y, group_z(g), ZQ)
            push(block, yq_send.at[t, d], yq_recv.at[t, d, g, 0], along_y[d])

    def begin(t):
        for d in range(2):
            push(piece(t, y, z, YP), yp_send.at[t, d], yp_recv.at[t, d, 0], along_y[d])
            push(piece(t, y, z, ZQ), zq_send.at[t, d], zq_recv.at[t, d, 0], along_z[d])
        send_zp(t, 1, 0, (z, z))
        send_yq(t, 0)

    def yp(t):
        for d in range(2):
            wait_for(piece(t, near_y[1 + d], z, YP), yp_recv.at[t, d, 0])
            push(piece(t, near_y[1 + d], z, YP, d), yp_send.at[t, d], yp_recv.at[t, d, 1], along_y[d])
        send_zp(t, 1, 1, (z, z))
        send_zp(t, 1, 2, (z, z))

    def yp_far(t):
        for d in range(2):
            wait_for(piece(t, near_y[3], z, YP, d), yp_recv.at[t, d, 1])
        send_zp(t, 1, 3, (z, z))

    def zq(t, k):
        for d in range(2):
            wait_for(piece(t, y, from_z(d, k), ZQ, d if k == 4 else None), zq_recv.at[t, d, k - 1])
            if k < 4:
                block = piece(t, y, from_z(d, k), ZQ, d if k == 3 else None)
                push(block, zq_send.at[t, d], zq_recv.at[t, d, k], along_z[d])
        send_yq(t, 2 * k - 1)
        if k < 4:
            send_yq(t, 2 * k)

    def zp(t, k, i):
        for d in range(2):
            block = piece(t, near_y[i], from_z(d, k), YP, d if k == 4 else None)
            wait_for(block, zp_recv.at[t, d, k - 1, i])
        if k < 4:
            send_zp(t, k + 1, i, (from_z(0, k), from_z(1, k)))

    def yq(t, g):
        for d in range(2):
            wait_for(piece(t, near_y[1 + d], group_z(g), ZQ), yq_recv.at[t, d, g, 0])
            block = piece(t, near_y[1 + d], group_z(g), ZQ, d)
            push(block, yq_send.at[t, d], yq_recv.at[t, d, g, 1], along_y[d])

    serves = core == y // 2
    dist = ((x - z_lo + NX) % NX, (z_lo - x + NX) % NX)
    side = (right, left)

    def served_part(t, kind, g, h):
        lane = pl.multiple_of(group_z(g) * GROUP + h * 128, 128)
        which = pl.ds(2, 1) if kind else pl.ds(0, 2)
        return served.at[t, which, :, pl.ds(lane, 128)]

    def make_picks():
        for i in range(2):
            unit = lax.broadcasted_iota(jnp.int32, (BLK, DN), 0)
            lane = lax.broadcasted_iota(jnp.int32, (BLK, DN), 1)
            wanted = unit + (BLK * (y % 2) + 64 * i)
            picks[i] = jnp.where(lane == wanted, 1.0, 0.0).astype(jnp.bfloat16)

    def cut(t, g):
        rows = pl.ds(pl.multiple_of(group_z(g) * GROUP, GROUP), GROUP)
        slot = g % 2
        kind = t % 2
        for m, lane in ((2, GU),) if kind else ((0, 0), (1, 640)):
            block = lax.dot_general(
                picks[m % 2],
                wall[t // 2, core, rows, lane : lane + DN],
                (((1,), (1,)), ((), ())),
                preferred_element_type=jnp.float32,
            ).astype(jnp.bfloat16)
            for h in range(2):
                stage[slot, h, m] = block[:, h * 128 : (h + 1) * 128]
        for h in range(2):
            src = stage.at[slot, h, pl.ds(2, 1) if kind else pl.ds(0, 2)]
            pltpu.make_async_copy(
                src, served_part(t // 2, kind, g, h), srecv.at[t * NZ + g, h]
            ).start()

    def pass_on(e, d):
        t, g = e // NZ, e % NZ

        @pl.when(serves)
        def _():
            for h in range(2):

                @pl.when(dist[h] == d)
                def _():
                    block = served_part(t // 2, t % 2, g, h)
                    wait_for(block, srecv.at[e, h])
                    if t < STREAMS - 1:
                        if d < 3:
                            push(block, s_fwd_send.at[t // 2, h], srecv.at[e, h], side[h])
                    elif d == 0:
                        for device in side:
                            push(block, s_last_send.at[h], srecv.at[e, h], device)
                    elif d == 1:
                        push(block, s_last_send.at[h], srecv.at[e, h], side[h])
                    push(block, s_d2d_send, s_d2d_recv, partner)

    def whole(t, g):
        for d in range(2):
            wait_for(piece(t, near_y[3], group_z(g), ZQ, d), yq_recv.at[t, d, g, 1])
        rows = pl.ds(pl.multiple_of(group_z(g) * GROUP, GROUP), GROUP)
        block = wall.at[t // 2, core, rows, pl.ds(*ALL[t % 2])]
        landed = d2d_recv.at[t // 2, g if t % 2 else NZ]
        push(block, d2d_send.at[t], landed, partner)

        @pl.when(jnp.logical_and(serves, x == z_lo))
        def _():
            cut(t, g)

    def normed(value):
        square = jnp.mean(value * value, axis=-1, keepdims=True)
        return (value * lax.rsqrt(square + EPS)).astype(jnp.bfloat16)

    halves = (pl.ds(0, HALF), pl.ds(HALF, HALF))

    def send_tokens(p):
        for i, device in enumerate((right, left)):
            for b in range(2):
                block = xa.at[p, x, halves[b]]
                remote(block, block, ag_send.at[p, i, b], ag_recv.at[p, i, b], device).start()

    def relay_tokens(p):
        for i, (device, origin) in enumerate(((right, x_l), (left, x_r))):
            block = xa.at[p, origin, halves[i]]
            wait_for(block, ag_recv.at[p, i, i])
            remote(block, block, ag_send.at[p, i, 2], ag_recv.at[p, i, 2], device).start()

    def await_tokens(p):
        for i, origin in enumerate((x_l, x_r)):
            wait_for(xa.at[p, origin, halves[1 - i]], ag_recv.at[p, i, 1 - i])
            wait_for(xa.at[p, x_far, halves[i]], ag_recv.at[p, i, 2])

    def hidden(t, c):
        tokens = xa[t].reshape(NX * TOK, D)
        pre[...] = jnp.dot(tokens, wall[t, c, :, :GU], preferred_element_type=jnp.float32)

        def rows_of(i, carry):
            rows = pl.ds(pl.multiple_of(i * HALF, HALF), HALF)
            gate = pre[rows, :DN] * IN_SCALE
            up = pltpu.roll(pre[rows, GU - DN :], DN - 64, 1) * IN_SCALE
            value = gate / (1.0 + jnp.exp(-gate)) * up
            lane = lax.broadcasted_iota(jnp.int32, value.shape, 1)
            hid[c, rows, :] = jnp.where(lane < COLS, value, 0.0).astype(jnp.bfloat16)
            return carry

        lax.fori_loop(0, NX * TOK // HALF, rows_of, 0)

    def columns(g):
        return pl.ds(pl.multiple_of(group_z(g) * CH, CH), CH)

    def down(t, j):
        drows = columns(j)
        wait_for(wall.at[t, 1 - core, drows, pl.ds(*ALL[1])], d2d_recv.at[t, j])
        total = None
        for c in range(2):
            term = lax.dot_general(
                hid[c],
                wall[t, c, drows, GU:],
                (((1,), (1,)), ((), ())),
                preferred_element_type=jnp.float32,
            )
            total = term if total is None else total + term
        accs[...] = (total * OUT_SCALE).reshape(NX, TOK, CH)
        own[:, drows] = accs[x]
        part[0, :, drows] = accs[x_r]
        part[1, :, drows] = accs[x_l]
        st2[t, :, drows] = accs[x_far].astype(jnp.bfloat16)
        for i, device in enumerate((right, left)):
            remote(
                st2.at[t, halves[i], drows],
                cbuf.at[t, i, :, drows],
                c_send.at[t, i, j],
                c_recv.at[t, i, j],
                device,
            ).start()

    def combine(t, j):
        drows = columns(j)
        for i, device in enumerate((right, left)):
            wait_for(cbuf.at[t, i, :, drows], c_recv.at[t, i, j])
            comb[t, i, halves[i], drows] = (
                part[i, halves[i], drows] + cbuf[t, i, :, drows].astype(jnp.float32)
            ).astype(jnp.bfloat16)
            comb[t, i, halves[1 - i], drows] = part[i, halves[1 - i], drows].astype(jnp.bfloat16)
            remote(
                comb.at[t, i, :, drows],
                rbuf.at[t, i, :, drows],
                r_send.at[t, i, j],
                r_recv.at[t, i, j],
                device,
            ).start()

    def finish(t):
        for j in range(NCH):
            for i in range(2):
                wait_for(rbuf.at[t, i, :, columns(j)], r_recv.at[t, i, j])
        branch = own[...] + rbuf[t, 0].astype(jnp.float32) + rbuf[t, 1].astype(jnp.float32)
        return (resid[...] + 0.5 * branch).astype(jnp.bfloat16)


    def compute(t, stage_of):
        if stage_of == 0:
            hidden(t, core)
        elif stage_of == 1:
            wait_for(wall.at[t, 1 - core, :, pl.ds(*ALL[0])], d2d_recv.at[t, NZ])
            hidden(t, 1 - core)

    def to_second():
        middle = finish(0).astype(jnp.float32)
        resid[...] = middle
        xa[1, x] = normed(middle)
        send_tokens(1)

    def first_tokens(p):
        start = prompt[...].astype(jnp.float32)
        resid[...] = start
        xa[p, x] = normed(start)
        send_tokens(p)

    def last_step():
        result[...] = finish(1)

    steps = dict(
        begin=begin,
        yp=yp,
        yp_far=yp_far,
        zq=zq,
        zp=zp,
        yq=yq,
        whole=whole,
        pass_on=pass_on,
        send_tokens=first_tokens,
        relay_tokens=relay_tokens,
        await_tokens=await_tokens,
        make_picks=make_picks,
        compute=compute,
        down=down,
        combine=combine,
        to_second=to_second,
        last_step=last_step,
    )
    for _, name, args in plan():
        steps[name](*args)

    def some(rows, lanes):
        return wall.at[0, 0, pl.ds(0, rows), pl.ds(*lanes)]

    for t in range(STREAMS):
        p_lanes, q_lanes = YP[t % 2], ZQ[t % 2]
        for d in range(2):
            wait_for(some(96, p_lanes), yp_send.at[t, d])
            wait_for(some(NZ * 96, q_lanes), yq_send.at[t, d])
            wait_for(some(224, q_lanes), zq_send.at[t, d])
            wait_for(some(NY * 224, p_lanes), zp_send.at[t, d])
        wait_for(some(D, ALL[t % 2]), d2d_send.at[t])
    for t in range(2):
        for i in range(2):
            for b in range(3):
                wait_for(xa.at[t, x, halves[0]], ag_send.at[t, i, b])
            for j in range(NCH):
                block = pl.ds(j * CH, CH)
                wait_for(st2.at[t, halves[i], block], c_send.at[t, i, j])
                wait_for(comb.at[t, i, :, block], r_send.at[t, i, j])

    @pl.when(serves)
    def _():
        for h in range(2):

            half = pl.ds(0, D // 2)

            @pl.when(dist[h] < 3)
            def _():
                wait_for(served.at[0, :, :, half], s_fwd_send.at[0, h])
                wait_for(served.at[0, pl.ds(0, 2), :, half], s_fwd_send.at[1, h])

            for d, sends in ((0, 2), (1, 1)):

                @pl.when(dist[h] == d)
                def _():
                    wait_for(served.at[0, pl.ds(0, sends), :, half], s_last_send.at[h])

        wait_for(served, s_d2d_send)

    @pl.when(jnp.logical_not(serves))
    def _():
        wait_for(served, s_d2d_recv)


def on_device(
    prompt,
    norm_first,
    gate_first,
    up_first,
    down_first,
    norm_second,
    gate_second,
    up_second,
    down_second,
):
    def pack(gain, gate, up, down):
        gain = gain[:, None]
        zero = jnp.zeros((ROWS, PACK - 3 * COLS), jnp.float32)
        return jnp.concatenate([gain * gate, gain * up, down, zero], axis=1).astype(jnp.bfloat16)

    packed = jnp.stack(
        [
            pack(norm_first, gate_first, up_first, down_first),
            pack(norm_second, gate_second, up_second, down_second),
        ]
    )
    dma = pltpu.SemaphoreType.DMA
    bf16, f32 = jnp.bfloat16, jnp.float32
    served, result = pl.pallas_call(
        kernel,
        out_shape=(
            jax.ShapeDtypeStruct((2, 3, BLK, D), bf16),
            jax.ShapeDtypeStruct((TOK, D), bf16),
        ),
        in_specs=[
            pl.BlockSpec(memory_space=pl.ANY),
            pl.BlockSpec(memory_space=pltpu.VMEM),
        ],
        out_specs=(
            pl.BlockSpec(memory_space=pl.ANY),
            pl.BlockSpec(memory_space=pltpu.VMEM),
        ),
        scratch_shapes=[
            pltpu.VMEM((2, 2, D, PACK), bf16),
            pltpu.VMEM((2, NX, TOK, D), bf16),
            pltpu.VMEM((NX * TOK, GU), f32),
            pltpu.VMEM((2, NX * TOK, DN), bf16),
            pltpu.VMEM((NX, TOK, CH), f32),
            pltpu.VMEM((TOK, D), f32),
            pltpu.VMEM((2, TOK, D), f32),
            pltpu.VMEM((2, TOK, D), bf16),
            pltpu.VMEM((2, 2, TOK, D), bf16),
            pltpu.VMEM((2, 2, HALF, D), bf16),
            pltpu.VMEM((2, 2, TOK, D), bf16),
            pltpu.VMEM((TOK, D), f32),
            pltpu.VMEM((2, 2, 3, BLK, 128), bf16),
            pltpu.VMEM((2, BLK, DN), bf16),
            dma((2,)),
            dma((STREAMS, 2, 2)),
            dma((STREAMS, 2)),
            dma((STREAMS, 2, 4)),
            dma((STREAMS, 2)),
            dma((STREAMS, 2, 4, NY)),
            dma((STREAMS, 2)),
            dma((STREAMS, 2, NZ, 2)),
            dma((STREAMS, 2)),
            dma((2, NZ + 1)),
            dma((STREAMS,)),
            dma((STREAMS * NZ, 2)),
            dma((2, 2)),
            dma((2,)),
            dma,
            dma,
            dma((2, 2, 3)),
            dma((2, 2, 3)),
            dma((2, 2, NCH)),
            dma((2, 2, NCH)),
            dma((2, 2, NCH)),
            dma((2, 2, NCH)),
        ],
        compiler_params=pltpu.CompilerParams(
            collective_id=0, has_side_effects=True, vmem_limit_bytes=66 * 1024 * 1000
        ),
    )(packed, prompt)
    blocks = [served[t, m].T for t in range(2) for m in range(3)]
    return (*blocks, result)


def solution(mesh):
    row = P(("gr", "fs"))
    tile = P(("gr", "fs"), "tp")
    token = P(("gr", "fs", "tp"), None)
    block = P(None, "fs")
    return jax.shard_map(
        on_device,
        mesh=mesh,
        in_specs=(token, row, tile, tile, tile, row, tile, tile, tile),
        out_specs=(block,) * 6 + (token,),
        check_vma=False,
    )
```
